128 devices in a mesh: ep: 32 (over z, y, core), tp: 4 (over x).
Axes of the slice: x: 4, y: 4, z: 4, core: 2. Of those that a mesh axis runs over, the one named last changes fastest.
Arguments:
- tokens: bfloat16 [16384, 2048], P(('ep', 'tp')), may hold values from -6 to 6
- norm_gain: float32 [2048], replicated, may hold values from 0.1 to 1.9
- w_gate: bfloat16 [128, 2048, 512], P(('ep', 'tp')), may hold values from -0.125 to 0.125
- w_up: bfloat16 [128, 2048, 512], P(('ep', 'tp')), may hold values from -0.125 to 0.125
- w_down: bfloat16 [128, 512, 2048], P(('ep', 'tp')), may hold values from -0.25 to 0.25
- routing: int32 [16384, 2], P(('ep', 'tp')), may hold values from 0 to 127, as said below
- gate_weight: float32 [16384, 2], P(('ep', 'tp')), may hold values from 0.05 to 1
Outputs:
- combined: bfloat16 [16384, 2048], P(('ep', 'tp'))
The draws below stay inside these ranges and needn't reach their ends.
Inputs may be any that keep to these rules, and one draw needn't show every extreme that they name: `routing`: A token's 2 experts are distinct and lie in one group of 4 consecutive experts. Of the 128 tokens of each device exactly 4 choose each group; no expert is named by more than 4 tokens of one device, and in every group one expert is named by exactly 4 tokens of every device.
All inputs are finite; a program needn't handle non-finite values.
Results may differ from the reference program's by a relative error of at most 0.0085.
Values may be sent and summed in bfloat16 or wider, within the bound.
No kernel may reach another device: no remote copies, remote signals or barrier semaphores. Data moves between devices by JAX's collectives and lax.ppermute only.
A program may use at most 64 MiB of HBM per device.

```python
import math
import jax
import jax.numpy as jnp
from jax import lax

D = 2048
FF = 512
GROUP_EXPERTS = 4
TOP = 2
TOK_DEV = 128
EXPERTS = 128
GROUPS = 32
CAP = 4
TOKENS = 16384


def draw_routing(key, part):
    source_count = TOKENS // TOK_DEV
    heavy_key = jax.random.fold_in(key, 11)
    cut_key = jax.random.fold_in(key, 12)
    shuffle_key = jax.random.fold_in(key, 13)
    heavy_member = jax.random.randint(heavy_key, (GROUPS,), 0, GROUP_EXPERTS)
    cut_points = jax.random.randint(cut_key, (source_count, GROUPS, 2), 0, CAP + 1)
    lower = jnp.min(cut_points, axis=-1)
    higher = jnp.max(cut_points, axis=-1)
    rest_loads = jnp.stack([lower, higher - lower, CAP - higher], axis=-1)
    members = jnp.arange(GROUP_EXPERTS, dtype=jnp.int32)
    is_heavy = members[None, :] == heavy_member[:, None]
    rank = jnp.clip(members[None, :] - (members[None, :] > heavy_member[:, None]).astype(jnp.int32), 0, 2)
    rank_full = jnp.broadcast_to(rank[None], (source_count, GROUPS, GROUP_EXPERTS))
    load_table = jnp.where(is_heavy[None], CAP, jnp.take_along_axis(rest_loads, rank_full, axis=2))
    bounds = jnp.cumsum(load_table, axis=-1)
    entries = jnp.arange(2 * CAP, dtype=jnp.int32)
    local_ident = jnp.sum((entries[None, None, :, None] >= bounds[:, :, None, :GROUP_EXPERTS - 1]).astype(jnp.int32), axis=-1)
    group_base = jnp.arange(GROUPS, dtype=jnp.int32) * GROUP_EXPERTS
    pair_table = jnp.stack([local_ident[:, :, :CAP], local_ident[:, :, CAP:]], axis=-1) + group_base[None, :, None, None]
    pair_table = pair_table.reshape(source_count, TOK_DEV, TOP)
    shuffles = jax.vmap(lambda subkey: jax.random.permutation(subkey, TOK_DEV))(jax.random.split(shuffle_key, source_count))
    routing = jnp.take_along_axis(pair_table, shuffles[:, :, None].astype(jnp.int32), axis=1)
    return routing.reshape(TOKENS, TOP).astype(jnp.int32)


def level_of(rng, shape, shards, low, top_value):
    level, own = 1.0, jax.random.fold_in(rng, 6)
    for dim, blocks in shards:
        steps = jnp.exp(jax.random.uniform(jax.random.fold_in(own, dim), (blocks,), jnp.float32, low / len(shards), top_value / len(shards)))
        level = level * jnp.repeat(steps, shape[dim] // blocks).reshape([-1 if axis == dim else 1 for axis in range(len(shape))])
    return level


def gaussian(rng, shape, spread, most, cuts=(), kind=jnp.bfloat16):
    values = spread * jax.random.normal(rng, shape, jnp.float32)
    if cuts:
        values = values * level_of(rng, shape, cuts, -0.22, 0.18)
    return jnp.clip(values, -most, most).astype(kind)


def setup_inputs(seed: int = 0) -> dict:
    key_list = jax.random.split(jax.random.key(seed), 8)
    tokens = gaussian(key_list[0], (TOKENS, D), 1.0, 6.0, ((0, 128),))
    norm_gain = jnp.clip(1.0 + 0.18 * jax.random.normal(key_list[1], (D,), jnp.float32), 0.1, 1.9)
    w_gate = gaussian(key_list[2], (EXPERTS, D, FF), D ** -0.5, 0.125, ((0, 128),))
    w_up = gaussian(key_list[3], (EXPERTS, D, FF), D ** -0.5, 0.125, ((0, 128),))
    w_down = gaussian(key_list[4], (EXPERTS, FF, D), FF ** -0.5, 0.25, ((0, 128),))
    routing = draw_routing(jax.random.fold_in(key_list[7], 71), 0)
    gate_weight = jnp.clip(jnp.exp(math.log(1.0) - 2.9957323 * jax.random.uniform(key_list[6], (TOKENS, TOP), jnp.float32) ** level_of(key_list[6], (TOKENS, TOP), ((0, 128),), -0.2, 0.2)), 0.05, 1.0)
    return {"tokens": tokens, "norm_gain": norm_gain, "w_gate": w_gate, "w_up": w_up, "w_down": w_down, "routing": routing, "gate_weight": gate_weight}


def reference(tokens, norm_gain, w_gate, w_up, w_down, routing, gate_weight):
    source_count = TOKENS // TOK_DEV
    values = tokens.astype(jnp.float32)
    scale = lax.rsqrt(lax.optimization_barrier(jnp.mean(values * values, axis=-1, keepdims=True)) + 1e-06)
    normed = (values * scale * norm_gain.astype(jnp.float32)).astype(jnp.bfloat16)
    assigned = routing.reshape(source_count, TOK_DEV * TOP).astype(jnp.int32)

    def count_slots(block):
        onehot = (block[:, None] == jnp.arange(EXPERTS, dtype=jnp.int32)[None, :]).astype(jnp.int32)
        running = jnp.cumsum(onehot, axis=0)
        return lax.optimization_barrier(jnp.sum(onehot * running, axis=1)) - 1
    slot_index = lax.map(count_slots, assigned)
    source_index = jnp.arange(source_count, dtype=jnp.int32)[:, None]
    position = (assigned * source_count + source_index) * CAP + slot_index
    dump_index = TOKENS * TOP
    slot_owner = jnp.full((EXPERTS * source_count * CAP,), dump_index, jnp.int32)
    slot_owner = slot_owner.at[position.reshape(-1)].set(jnp.arange(TOKENS * TOP, dtype=jnp.int32))
    slot_owner = slot_owner.reshape(EXPERTS, source_count * CAP)
    normed_pad = jnp.concatenate([normed, jnp.zeros((1, D), jnp.bfloat16)], axis=0)

    def one_expert(expert, results):
        owners = lax.dynamic_index_in_dim(slot_owner, expert, 0, keepdims=False)
        slot_rows = normed_pad[owners // TOP]
        gate_part = jnp.dot(slot_rows, lax.dynamic_index_in_dim(w_gate, expert, 0, keepdims=False), preferred_element_type=jnp.float32)
        up_part = jnp.dot(slot_rows, lax.dynamic_index_in_dim(w_up, expert, 0, keepdims=False), preferred_element_type=jnp.float32)
        hidden = (jax.nn.silu(gate_part) * up_part).astype(jnp.bfloat16)
        expert_out = jnp.dot(hidden, lax.dynamic_index_in_dim(w_down, expert, 0, keepdims=False), preferred_element_type=jnp.float32).astype(jnp.bfloat16)
        return results.at[owners].set(expert_out)
    results = lax.fori_loop(0, EXPERTS, one_expert, jnp.zeros((TOKENS * TOP + 1, D), jnp.bfloat16))
    picked = results[:TOKENS * TOP].reshape(TOKENS, TOP, D).astype(jnp.float32)
    return lax.optimization_barrier(jnp.sum(gate_weight.astype(jnp.float32)[:, :, None] * picked, axis=1)).astype(jnp.bfloat16)
```

```python
import jax
import jax.numpy as jnp
from jax import lax
from jax.experimental import pallas as pl
from jax.experimental.pallas import tpu as pltpu
from jax.sharding import PartitionSpec as P

AXES = ("ep", "tp")
BF = jnp.bfloat16
F32 = jnp.float32


def rank_in_group(group, groups):
    n = group.shape[1]
    member = lax.broadcasted_iota(jnp.int32, (groups, n), 0) == group
    earlier = lax.broadcasted_iota(jnp.int32, (n, n), 0) < lax.broadcasted_iota(jnp.int32, (n, n), 1)
    counts = jnp.dot(member.astype(BF), earlier.astype(BF), preferred_element_type=F32)
    return jnp.sum(jnp.where(member, counts, 0.0), axis=0, keepdims=True).astype(jnp.int32)


def dispatch_kernel(groups, members, tok_ref, gain_ref, route_ref, out_ref):
    rows, width = tok_ref.shape
    slots = rows // groups
    group = route_ref[0:1, :] // members
    place = group * slots + rank_in_group(group, groups)
    pick = (lax.broadcasted_iota(jnp.int32, (rows, rows), 0) == place).astype(BF)
    values = tok_ref[...].astype(F32)
    scale = lax.rsqrt(jnp.mean(values * values, axis=-1, keepdims=True) + 1e-06)
    normed = (values * scale * gain_ref[...]).astype(BF)
    ordered = jnp.dot(pick, normed, preferred_element_type=F32).astype(BF)
    ordered = ordered.reshape(groups, slots, width)
    for m in range(members):
        out_ref[:, m] = ordered


def expert_kernel(x_ref, wg_ref, wu_ref, wd_ref, out_ref):
    blocks, slots, width = x_ref.shape
    step = blocks // 2
    for c in range(2):
        x = x_ref[c * step:(c + 1) * step].reshape(step * slots, width)
        gate = jnp.dot(x, wg_ref[...], preferred_element_type=F32)
        up = jnp.dot(x, wu_ref[...], preferred_element_type=F32)
        hidden = (gate / (1.0 + jnp.exp(-gate)) * up).astype(BF)
        out = jnp.dot(hidden, wd_ref[...], preferred_element_type=F32).astype(BF)
        out_ref[c * step:(c + 1) * step] = out.reshape(step, slots, width)


def combine_kernel(groups, members, r_ref, route_ref, gw_ref, out_ref):
    blocks, slots, width = r_ref.shape
    rows = out_ref.shape[0]
    e0, e1 = route_ref[0:1, :], route_ref[1:2, :]
    rank = rank_in_group(e0 // members, groups)
    row = lax.broadcasted_iota(jnp.int32, (blocks * slots, rows), 0)
    expert = row // slots
    weight = jnp.where(expert == e0, gw_ref[0:1, :], 0.0) + jnp.where(expert == e1, gw_ref[1:2, :], 0.0)
    weight = jnp.where(row % slots == rank, weight, 0.0)
    high = weight.astype(BF)
    low = (weight - high.astype(F32)).astype(BF)
    both = jnp.concatenate([high, low], axis=1)
    r = r_ref[...].reshape(blocks * slots, width)
    out = lax.dot_general(both, r, (((0,), (0,)), ((), ())), preferred_element_type=F32)
    out_ref[...] = (out[:rows] + out[rows:]).astype(BF)


def local(tokens, norm_gain, w_gate, w_up, w_down, routing, gate_weight):
    rows, width = tokens.shape
    groups = lax.axis_size("ep")
    members = lax.axis_size("tp")
    experts = groups * members
    slots = rows // groups
    route = routing.T
    weights = gate_weight.T
    params = pltpu.CompilerParams(vmem_limit_bytes=48 * 1024 * 1024)
    outgoing = pl.pallas_call(
        lambda *refs: dispatch_kernel(groups, members, *refs),
        out_shape=jax.ShapeDtypeStruct((groups, members, slots, width), BF),
        compiler_params=params,
        name="dispatch",
    )(tokens, norm_gain.reshape(1, width), route)
    arrived = lax.all_to_all(outgoing.reshape(experts, slots, width), AXES, split_axis=0, concat_axis=0, tiled=True)
    answered = pl.pallas_call(
        expert_kernel,
        out_shape=jax.ShapeDtypeStruct((experts, slots, width), BF),
        compiler_params=params,
        name="expert",
    )(arrived, w_gate[0], w_up[0], w_down[0])
    returned = lax.all_to_all(answered, AXES, split_axis=0, concat_axis=0, tiled=True)
    return pl.pallas_call(
        lambda *refs: combine_kernel(groups, members, *refs),
        out_shape=jax.ShapeDtypeStruct((rows, width), BF),
        compiler_params=params,
        name="combine",
    )(returned, route, weights)


def solution(mesh):
    placed = (
        P(AXES, None),
        P(),
        P(AXES, None, None),
        P(AXES, None, None),
        P(AXES, None, None),
        P(AXES, None),
        P(AXES, None),
    )
    return jax.shard_map(local, mesh=mesh, in_specs=placed, out_specs=P(AXES, None), check_vma=False)
```

```python
import jax
import jax.numpy as jnp
from jax import lax
from jax.experimental import pallas as pl
from jax.experimental.pallas import tpu as pltpu
from jax.sharding import PartitionSpec as P

AXES = ("ep", "tp")
BF = jnp.bfloat16
F32 = jnp.float32


def rank_in_group(group, groups):
    n = group.shape[1]
    member = lax.broadcasted_iota(jnp.int32, (groups, n), 0) == group
    earlier = lax.broadcasted_iota(jnp.int32, (n, n), 0) < lax.broadcasted_iota(jnp.int32, (n, n), 1)
    counts = jnp.dot(member.astype(BF), earlier.astype(BF), preferred_element_type=F32)
    return jnp.sum(jnp.where(member, counts, 0.0), axis=0, keepdims=True).astype(jnp.int32)


def dispatch_kernel(groups, members, tok_ref, gain_ref, route_ref, out_ref):
    rows, width = tok_ref.shape
    slots = rows // groups
    group = route_ref[0:1, :] // members
    place = group * slots + rank_in_group(group, groups)
    pick = (lax.broadcasted_iota(jnp.int32, (rows, rows), 0) == place).astype(BF)
    values = tok_ref[...].astype(F32)
    scale = lax.rsqrt(jnp.mean(values * values, axis=-1, keepdims=True) + 1e-06)
    normed = (values * scale * gain_ref[...]).astype(BF)
    ordered = jnp.dot(pick, normed, preferred_element_type=F32).astype(BF)
    ordered = ordered.reshape(groups, slots, width)
    for m in range(members):
        out_ref[:, m] = ordered


def expert_kernel(x_ref, wg_ref, wu_ref, wd_ref, out_ref):
    blocks, slots, width = x_ref.shape
    step = blocks // 2
    half = wg_ref.shape[1] // 2
    for c in range(2):
        x = x_ref[c * step:(c + 1) * step].reshape(step * slots, width)
        parts = []
        for n in range(2):
            gate = jnp.dot(x, wg_ref[:, n * half:(n + 1) * half], preferred_element_type=F32)
            up = jnp.dot(x, wu_ref[:, n * half:(n + 1) * half], preferred_element_type=F32)
            parts.append((gate / (1.0 + jnp.exp(-gate)) * up).astype(BF))
        hidden = jnp.concatenate(parts, axis=1)
        out = jnp.dot(hidden, wd_ref[...], preferred_element_type=F32).astype(BF)
        out_ref[c * step:(c + 1) * step] = out.reshape(step, slots, width)


def combine_kernel(groups, members, r_ref, route_ref, gw_ref, out_ref):
    blocks, slots, width = r_ref.shape
    rows = out_ref.shape[0]
    e0, e1 = route_ref[0:1, :], route_ref[1:2, :]
    rank = rank_in_group(e0 // members, groups)
    row = lax.broadcasted_iota(jnp.int32, (blocks * slots, rows), 0)
    expert = row // slots
    weight = jnp.where(expert == e0, gw_ref[0:1, :], 0.0) + jnp.where(expert == e1, gw_ref[1:2, :], 0.0)
    weight = jnp.where(row % slots == rank, weight, 0.0)
    high = weight.astype(BF)
    low = (weight - high.astype(F32)).astype(BF)
    both = jnp.concatenate([high, low], axis=1)
    r = r_ref[...].reshape(blocks * slots, width)
    out = lax.dot_general(both, r, (((0,), (0,)), ((), ())), preferred_element_type=F32)
    out_ref[...] = (out[:rows] + out[rows:]).astype(BF)


def local(tokens, norm_gain, w_gate, w_up, w_down, routing, gate_weight):
    rows, width = tokens.shape
    groups = lax.axis_size("ep")
    members = lax.axis_size("tp")
    experts = groups * members
    slots = rows // groups
    route = routing.T
    weights = gate_weight.T
    params = pltpu.CompilerParams(vmem_limit_bytes=20 * 1024 * 1024)
    outgoing = pl.pallas_call(
        lambda *refs: dispatch_kernel(groups, members, *refs),
        out_shape=jax.ShapeDtypeStruct((groups, members, slots, width), BF),
        compiler_params=params,
        name="dispatch",
    )(tokens, norm_gain.reshape(1, width), route)
    arrived = lax.all_to_all(outgoing.reshape(experts, slots, width), AXES, split_axis=0, concat_axis=0, tiled=True)
    in_vmem = pl.BlockSpec(memory_space=pltpu.VMEM)
    answered = pl.pallas_call(
        expert_kernel,
        in_specs=[in_vmem] * 4,
        out_specs=in_vmem,
        out_shape=jax.ShapeDtypeStruct((experts, slots, width), BF),
        compiler_params=params,
        name="expert",
    )(arrived, w_gate[0], w_up[0], w_down[0])
    returned = lax.all_to_all(answered, AXES, split_axis=0, concat_axis=0, tiled=True)
    return pl.pallas_call(
        lambda *refs: combine_kernel(groups, members, *refs),
        out_shape=jax.ShapeDtypeStruct((rows, width), BF),
        compiler_params=params,
        name="combine",
    )(returned, route, weights)


def solution(mesh):
    placed = (
        P(AXES, None),
        P(),
        P(AXES, None, None),
        P(AXES, None, None),
        P(AXES, None, None),
        P(AXES, None),
        P(AXES, None),
    )
    return jax.shard_map(local, mesh=mesh, in_specs=placed, out_specs=P(AXES, None), check_vma=False)
```

```python
import jax
import jax.numpy as jnp
from jax import lax
from jax.experimental import pallas as pl
from jax.experimental.pallas import tpu as pltpu
from jax.sharding import PartitionSpec as P

AXES = ("ep", "tp")
BF = jnp.bfloat16
F32 = jnp.float32


def rank_in_group(group, groups):
    n = group.shape[1]
    member = lax.broadcasted_iota(jnp.int32, (groups, n), 0) == group
    earlier = lax.broadcasted_iota(jnp.int32, (n, n), 0) < lax.broadcasted_iota(jnp.int32, (n, n), 1)
    counts = jnp.dot(member.astype(BF), earlier.astype(BF), preferred_element_type=F32)
    return jnp.sum(jnp.where(member, counts, 0.0), axis=0, keepdims=True).astype(jnp.int32)


def slots_kernel(groups, members, route_ref, pick_ref):
    rows = pick_ref.shape[0]
    group = route_ref[0:1, :] // members
    place = group * (rows // groups) + rank_in_group(group, groups)
    pick_ref[...] = (lax.broadcasted_iota(jnp.int32, (rows, rows), 0) == place).astype(BF)


def dispatch_kernel(groups, members, pick_ref, tok_ref, gain_ref, out_ref):
    rows, width = tok_ref.shape
    values = tok_ref[...].astype(F32)
    scale = lax.rsqrt(jnp.mean(values * values, axis=-1, keepdims=True) + 1e-06)
    normed = (values * scale * gain_ref[...]).astype(BF)
    ordered = jnp.dot(pick_ref[...], normed, preferred_element_type=F32).astype(BF)
    ordered = ordered.reshape(groups, rows // groups, width)
    for m in range(members):
        out_ref[:, m] = ordered


def selection(groups, members, slots, route_ref, gw_ref):
    rows = route_ref.shape[1]
    e0, e1 = route_ref[0:1, :], route_ref[1:2, :]
    rank = rank_in_group(e0 // members, groups)
    row = lax.broadcasted_iota(jnp.int32, (groups * members * slots, rows), 0)
    expert = row // slots
    weight = jnp.where(expert == e0, gw_ref[0:1, :], 0.0) + jnp.where(expert == e1, gw_ref[1:2, :], 0.0)
    weight = jnp.where(row % slots == rank, weight, 0.0).T
    high = weight.astype(BF)
    return jnp.concatenate([high, (weight - high.astype(F32)).astype(BF)], axis=0)


def expert_kernel(groups, members, x_ref, wg_ref, wu_ref, wd_ref, route_ref, gw_ref, out_ref, pick_ref):
    pick_ref[...] = selection(groups, members, x_ref.shape[1], route_ref, gw_ref)
    blocks, slots, width = x_ref.shape
    step = blocks // 2
    half = wg_ref.shape[1] // 2
    for c in range(2):
        x = x_ref[c * step:(c + 1) * step].reshape(step * slots, width)
        parts = []
        for n in range(2):
            gate = jnp.dot(x, wg_ref[:, n * half:(n + 1) * half], preferred_element_type=F32)
            up = jnp.dot(x, wu_ref[:, n * half:(n + 1) * half], preferred_element_type=F32)
            parts.append((gate / (1.0 + jnp.exp(-gate)) * up).astype(BF))
        hidden = jnp.concatenate(parts, axis=1)
        out = jnp.dot(hidden, wd_ref[...], preferred_element_type=F32).astype(BF)
        out_ref[c * step:(c + 1) * step] = out.reshape(step, slots, width)


def combine_kernel(r_ref, pick_ref, out_ref):
    blocks, slots, width = r_ref.shape
    rows = out_ref.shape[0]
    r = r_ref[...].reshape(blocks * slots, width)
    out = jnp.dot(pick_ref[...], r, preferred_element_type=F32)
    out_ref[...] = (out[:rows] + out[rows:]).astype(BF)


def local(tokens, norm_gain, w_gate, w_up, w_down, routing, gate_weight):
    rows, width = tokens.shape
    groups = lax.axis_size("ep")
    members = lax.axis_size("tp")
    experts = groups * members
    slots = rows // groups
    route = routing.T
    weights = gate_weight.T
    params = pltpu.CompilerParams(vmem_limit_bytes=20 * 1024 * 1024)
    pick = pl.pallas_call(
        lambda *refs: slots_kernel(groups, members, *refs),
        out_shape=jax.ShapeDtypeStruct((rows, rows), BF),
        compiler_params=params,
        cost_estimate=pl.CostEstimate(flops=2_000_000_000, bytes_accessed=0, transcendentals=0),
        name="slots",
    )(route)
    outgoing = pl.pallas_call(
        lambda *refs: dispatch_kernel(groups, members, *refs),
        out_shape=jax.ShapeDtypeStruct((groups, members, slots, width), BF),
        compiler_params=params,
        name="dispatch",
    )(pick, tokens, norm_gain.reshape(1, width))
    arrived = lax.all_to_all(outgoing.reshape(experts, slots, width), AXES, split_axis=0, concat_axis=0, tiled=True)
    in_vmem = pl.BlockSpec(memory_space=pltpu.VMEM)
    answered, weighted = pl.pallas_call(
        lambda *refs: expert_kernel(groups, members, *refs),
        in_specs=[in_vmem] * 6,
        out_specs=[in_vmem] * 2,
        out_shape=[
            jax.ShapeDtypeStruct((experts, slots, width), BF),
            jax.ShapeDtypeStruct((2 * rows, experts * slots), BF),
        ],
        compiler_params=params,
        name="expert",
    )(arrived, w_gate[0], w_up[0], w_down[0], route, weights)
    returned = lax.all_to_all(answered, AXES, split_axis=0, concat_axis=0, tiled=True)
    return pl.pallas_call(
        combine_kernel,
        out_shape=jax.ShapeDtypeStruct((rows, width), BF),
        compiler_params=params,
        name="combine",
    )(returned, weighted)


def solution(mesh):
    placed = (
        P(AXES, None),
        P(),
        P(AXES, None, None),
        P(AXES, None, None),
        P(AXES, None, None),
        P(AXES, None),
        P(AXES, None),
    )
    return jax.shard_map(local, mesh=mesh, in_specs=placed, out_specs=P(AXES, None), check_vma=False)
```

```python
import jax
import jax.numpy as jnp
from jax import lax
from jax.experimental import pallas as pl
from jax.experimental.pallas import tpu as pltpu
from jax.sharding import PartitionSpec as P

AXES = ("ep", "tp")
BF = jnp.bfloat16
F32 = jnp.float32


def rank_in_group(group, groups):
    n = group.shape[1]
    member = lax.broadcasted_iota(jnp.int32, (groups, n), 0) == group
    earlier = lax.broadcasted_iota(jnp.int32, (n, n), 0) < lax.broadcasted_iota(jnp.int32, (n, n), 1)
    counts = jnp.dot(member.astype(BF), earlier.astype(BF), preferred_element_type=F32)
    return jnp.sum(jnp.where(member, counts, 0.0), axis=0, keepdims=True).astype(jnp.int32)


def lead_kernel(out_ref):
    out_ref[...] = jnp.zeros(out_ref.shape, jnp.int32)


def slots_kernel(groups, members, zero_ref, route_ref, pick_ref):
    rows = pick_ref.shape[0]
    group = (route_ref[0:1, :] + zero_ref[0:1, :]) // members
    place = group * (rows // groups) + rank_in_group(group, groups)
    pick_ref[...] = (lax.broadcasted_iota(jnp.int32, (rows, rows), 0) == place).astype(BF)


def dispatch_kernel(groups, members, pick_ref, tok_ref, gain_ref, out_ref):
    rows, width = tok_ref.shape
    values = tok_ref[...].astype(F32)
    scale = lax.rsqrt(jnp.mean(values * values, axis=-1, keepdims=True) + 1e-06)
    normed = (values * scale * gain_ref[...]).astype(BF)
    ordered = jnp.dot(pick_ref[...], normed, preferred_element_type=F32).astype(BF)
    ordered = ordered.reshape(groups, rows // groups, width)
    for m in range(members):
        out_ref[:, m] = ordered


def selection(groups, members, slots, route_ref, gw_ref):
    rows = route_ref.shape[1]
    e0, e1 = route_ref[0:1, :], route_ref[1:2, :]
    rank = rank_in_group(e0 // members, groups)
    row = lax.broadcasted_iota(jnp.int32, (groups * members * slots, rows), 0)
    expert = row // slots
    weight = jnp.where(expert == e0, gw_ref[0:1, :], 0.0) + jnp.where(expert == e1, gw_ref[1:2, :], 0.0)
    weight = jnp.where(row % slots == rank, weight, 0.0).T
    high = weight.astype(BF)
    return jnp.concatenate([high, (weight - high.astype(F32)).astype(BF)], axis=0)


def expert_kernel(groups, members, x_ref, wg_ref, wu_ref, wd_ref, route_ref, gw_ref, out_ref, pick_ref):
    pick_ref[...] = selection(groups, members, x_ref.shape[1], route_ref, gw_ref)
    blocks, slots, width = x_ref.shape
    step = blocks // 2
    half = wg_ref.shape[1] // 2
    for c in range(2):
        x = x_ref[c * step:(c + 1) * step].reshape(step * slots, width)
        parts = []
        for n in range(2):
            gate = jnp.dot(x, wg_ref[:, n * half:(n + 1) * half], preferred_element_type=F32)
            up = jnp.dot(x, wu_ref[:, n * half:(n + 1) * half], preferred_element_type=F32)
            parts.append((gate / (1.0 + jnp.exp(-gate)) * up).astype(BF))
        hidden = jnp.concatenate(parts, axis=1)
        out = jnp.dot(hidden, wd_ref[...], preferred_element_type=F32).astype(BF)
        out_ref[c * step:(c + 1) * step] = out.reshape(step, slots, width)


def combine_kernel(r_ref, pick_ref, out_hbm, out_ref, sems):
    blocks, slots, width = r_ref.shape
    rows = out_ref.shape[0]
    parts = sems.shape[0]
    step = width // parts
    pick = pick_ref[...]
    copies = []
    for p in range(parts):
        span = pl.ds(p * step, step)
        r = r_ref[:, :, p * step:(p + 1) * step].reshape(blocks * slots, step)
        out = jnp.dot(pick, r, preferred_element_type=F32)
        out_ref[:, p * step:(p + 1) * step] = (out[:rows] + out[rows:]).astype(BF)
        copies.append(pltpu.make_async_copy(out_ref.at[:, span], out_hbm.at[:, span], sems.at[p]))
        copies[-1].start()
    for copy in copies:
        copy.wait()


def local(tokens, norm_gain, w_gate, w_up, w_down, routing, gate_weight):
    rows, width = tokens.shape
    groups = lax.axis_size("ep")
    members = lax.axis_size("tp")
    experts = groups * members
    slots = rows // groups
    route = routing.T
    weights = gate_weight.T
    params = pltpu.CompilerParams(vmem_limit_bytes=20 * 1024 * 1024)
    busy = pl.CostEstimate(flops=2_000_000_000, bytes_accessed=0, transcendentals=0)
    zero = pl.pallas_call(
        lead_kernel,
        out_shape=jax.ShapeDtypeStruct((8, rows), jnp.int32),
        compiler_params=params,
        cost_estimate=busy,
        name="lead",
    )()
    pick = pl.pallas_call(
        lambda *refs: slots_kernel(groups, members, *refs),
        out_shape=jax.ShapeDtypeStruct((rows, rows), BF),
        compiler_params=params,
        name="slots",
    )(zero, route)
    outgoing = pl.pallas_call(
        lambda *refs: dispatch_kernel(groups, members, *refs),
        out_shape=jax.ShapeDtypeStruct((groups, members, slots, width), BF),
        compiler_params=params,
        name="dispatch",
    )(pick, tokens, norm_gain.reshape(1, width))
    arrived = lax.all_to_all(outgoing.reshape(experts, slots, width), AXES, split_axis=0, concat_axis=0, tiled=True)
    in_vmem = pl.BlockSpec(memory_space=pltpu.VMEM)
    answered, weighted = pl.pallas_call(
        lambda *refs: expert_kernel(groups, members, *refs),
        in_specs=[in_vmem] * 6,
        out_specs=[in_vmem] * 2,
        out_shape=[
            jax.ShapeDtypeStruct((experts, slots, width), BF),
            jax.ShapeDtypeStruct((2 * rows, experts * slots), BF),
        ],
        compiler_params=params,
        name="expert",
    )(arrived, w_gate[0], w_up[0], w_down[0], route, weights)
    returned = lax.all_to_all(answered, AXES, split_axis=0, concat_axis=0, tiled=True)
    return pl.pallas_call(
        combine_kernel,
        in_specs=[in_vmem] * 2,
        out_specs=pl.BlockSpec(memory_space=pltpu.HBM),
        out_shape=jax.ShapeDtypeStruct((rows, width), BF),
        scratch_shapes=[pltpu.VMEM((rows, width), BF), pltpu.SemaphoreType.DMA((4,))],
        compiler_params=params,
        name="combine",
    )(returned, weighted)


def solution(mesh):
    placed = (
        P(AXES, None),
        P(),
        P(AXES, None, None),
        P(AXES, None, None),
        P(AXES, None, None),
        P(AXES, None),
        P(AXES, None),
    )
    return jax.shard_map(local, mesh=mesh, in_specs=placed, out_specs=P(AXES, None), check_vma=False)
```

```python
import jax
import jax.numpy as jnp
from jax import lax
from jax.experimental import pallas as pl
from jax.experimental.pallas import tpu as pltpu
from jax.sharding import PartitionSpec as P

AXES = ("ep", "tp")
BF = jnp.bfloat16
F32 = jnp.float32


def rank_in_group(group, groups):
    n = group.shape[1]
    member = lax.broadcasted_iota(jnp.int32, (groups, n), 0) == group
    earlier = lax.broadcasted_iota(jnp.int32, (n, n), 0) < lax.broadcasted_iota(jnp.int32, (n, n), 1)
    counts = jnp.dot(member.astype(BF), earlier.astype(BF), preferred_element_type=F32)
    return jnp.sum(jnp.where(member, counts, 0.0), axis=0, keepdims=True).astype(jnp.int32)


def dispatch_kernel(groups, members, tok_hbm, gain_hbm, route_hbm, out_ref, tok_ref, gain_ref, route_ref, sems):
    rows, width = tok_ref.shape
    slots = rows // groups
    copies = [
        pltpu.make_async_copy(route_hbm, route_ref, sems.at[0]),
        pltpu.make_async_copy(tok_hbm, tok_ref, sems.at[1]),
        pltpu.make_async_copy(gain_hbm, gain_ref, sems.at[2]),
    ]
    for copy in copies:
        copy.start()
    copies[0].wait()
    group = route_ref[0:1, :] // members
    place = group * slots + rank_in_group(group, groups)
    pick = (lax.broadcasted_iota(jnp.int32, (rows, rows), 0) == place).astype(BF)
    copies[1].wait()
    copies[2].wait()
    half = rows // 2
    for c in range(2):
        values = jnp.dot(pick[c * half:(c + 1) * half], tok_ref[...], preferred_element_type=F32)
        scale = lax.rsqrt(jnp.mean(values * values, axis=-1, keepdims=True) + 1e-06)
        normed = (values * scale * gain_ref[...]).astype(BF).reshape(groups // 2, slots, width)
        for m in range(members):
            out_ref[c * groups // 2:(c + 1) * groups // 2, m] = normed


def selection(groups, members, slots, route_ref, gw_ref):
    rows = route_ref.shape[1]
    e0, e1 = route_ref[0:1, :], route_ref[1:2, :]
    rank = rank_in_group(e0 // members, groups)
    row = lax.broadcasted_iota(jnp.int32, (groups * members * slots, rows), 0)
    expert = row // slots
    weight = jnp.where(expert == e0, gw_ref[0:1, :], 0.0) + jnp.where(expert == e1, gw_ref[1:2, :], 0.0)
    weight = jnp.where(row % slots == rank, weight, 0.0).T
    high = weight.astype(BF)
    return jnp.concatenate([high, (weight - high.astype(F32)).astype(BF)], axis=0)


def expert_kernel(groups, members, x_ref, wg_ref, wu_ref, wd_ref, route_ref, gw_ref, out_ref, pick_ref):
    pick_ref[...] = selection(groups, members, x_ref.shape[1], route_ref, gw_ref)
    blocks, slots, width = x_ref.shape
    step = blocks // 2
    half = wg_ref.shape[1] // 2
    for c in range(2):
        x = x_ref[c * step:(c + 1) * step].reshape(step * slots, width)
        parts = []
        for n in range(2):
            gate = jnp.dot(x, wg_ref[:, n * half:(n + 1) * half], preferred_element_type=F32)
            up = jnp.dot(x, wu_ref[:, n * half:(n + 1) * half], preferred_element_type=F32)
            parts.append((gate / (1.0 + jnp.exp(-gate)) * up).astype(BF))
        hidden = jnp.concatenate(parts, axis=1)
        out = jnp.dot(hidden, wd_ref[...], preferred_element_type=F32).astype(BF)
        out_ref[c * step:(c + 1) * step] = out.reshape(step, slots, width)


def combine_kernel(r_ref, pick_ref, out_hbm, out_ref, sems):
    blocks, slots, width = r_ref.shape
    rows = out_ref.shape[0]
    parts = sems.shape[0]
    step = width // parts
    pick = pick_ref[...]
    copies = []
    for p in range(parts):
        span = pl.ds(p * step, step)
        r = r_ref[:, :, p * step:(p + 1) * step].reshape(blocks * slots, step)
        out = jnp.dot(pick, r, preferred_element_type=F32)
        out_ref[:, p * step:(p + 1) * step] = (out[:rows] + out[rows:]).astype(BF)
        copies.append(pltpu.make_async_copy(out_ref.at[:, span], out_hbm.at[:, span], sems.at[p]))
        copies[-1].start()
    for copy in copies:
        copy.wait()


def local(tokens, norm_gain, w_gate, w_up, w_down, routing, gate_weight):
    rows, width = tokens.shape
    groups = lax.axis_size("ep")
    members = lax.axis_size("tp")
    experts = groups * members
    slots = rows // groups
    route = routing.T
    weights = gate_weight.T
    params = pltpu.CompilerParams(vmem_limit_bytes=20 * 1024 * 1024)
    in_vmem = pl.BlockSpec(memory_space=pltpu.VMEM)
    in_hbm = pl.BlockSpec(memory_space=pltpu.HBM)
    sources = [pltpu.with_memory_space_constraint(v, pltpu.HBM) for v in (tokens, norm_gain.reshape(1, width), route)]
    outgoing = pl.pallas_call(
        lambda *refs: dispatch_kernel(groups, members, *refs),
        in_specs=[in_hbm] * 3,
        out_specs=in_vmem,
        out_shape=jax.ShapeDtypeStruct((groups, members, slots, width), BF),
        scratch_shapes=[
            pltpu.VMEM((rows, width), BF),
            pltpu.VMEM((1, width), F32),
            pltpu.VMEM(route.shape, jnp.int32),
            pltpu.SemaphoreType.DMA((3,)),
        ],
        compiler_params=params,
        name="dispatch",
    )(*sources)
    arrived = lax.all_to_all(outgoing.reshape(experts, slots, width), AXES, split_axis=0, concat_axis=0, tiled=True)
    answered, weighted = pl.pallas_call(
        lambda *refs: expert_kernel(groups, members, *refs),
        in_specs=[in_vmem] * 6,
        out_specs=[in_vmem] * 2,
        out_shape=[
            jax.ShapeDtypeStruct((experts, slots, width), BF),
            jax.ShapeDtypeStruct((2 * rows, experts * slots), BF),
        ],
        compiler_params=params,
        name="expert",
    )(arrived, w_gate[0], w_up[0], w_down[0], route, weights)
    returned = lax.all_to_all(answered, AXES, split_axis=0, concat_axis=0, tiled=True)
    return pl.pallas_call(
        combine_kernel,
        in_specs=[in_vmem] * 2,
        out_specs=pl.BlockSpec(memory_space=pltpu.HBM),
        out_shape=jax.ShapeDtypeStruct((rows, width), BF),
        scratch_shapes=[pltpu.VMEM((rows, width), BF), pltpu.SemaphoreType.DMA((4,))],
        compiler_params=params,
        name="combine",
    )(returned, weighted)


def solution(mesh):
    placed = (
        P(AXES, None),
        P(),
        P(AXES, None, None),
        P(AXES, None, None),
        P(AXES, None, None),
        P(AXES, None),
        P(AXES, None),
    )
    return jax.shard_map(local, mesh=mesh, in_specs=placed, out_specs=P(AXES, None), check_vma=False)
```

```python
import jax
import jax.numpy as jnp
from jax import lax
from jax.experimental import pallas as pl
from jax.experimental.pallas import tpu as pltpu
from jax.sharding import PartitionSpec as P

AXES = ("ep", "tp")
BF = jnp.bfloat16
F32 = jnp.float32


def rank_in_group(group, groups):
    n = group.shape[1]
    member = lax.broadcasted_iota(jnp.int32, (groups, n), 0) == group
    earlier = lax.broadcasted_iota(jnp.int32, (n, n), 0) < lax.broadcasted_iota(jnp.int32, (n, n), 1)
    counts = jnp.dot(member.astype(BF), earlier.astype(BF), preferred_element_type=F32)
    return jnp.sum(jnp.where(member, counts, 0.0), axis=0, keepdims=True).astype(jnp.int32)


def lead_kernel(out_ref):
    out_ref[...] = jnp.zeros(out_ref.shape, jnp.int32)


def slots_kernel(groups, members, zero_ref, route_ref, pick_ref):
    rows = pick_ref.shape[0]
    group = (route_ref[0:1, :] + zero_ref[0:1, :]) // members
    place = group * (rows // groups) + rank_in_group(group, groups)
    pick_ref[...] = (lax.broadcasted_iota(jnp.int32, (rows, rows), 0) == place).astype(BF)


def dispatch_kernel(groups, members, pick_ref, tok_ref, gain_ref, out_ref):
    rows, width = tok_ref.shape
    half = rows // 2
    for c in range(2):
        values = jnp.dot(pick_ref[c * half:(c + 1) * half], tok_ref[...], preferred_element_type=F32)
        scale = lax.rsqrt(jnp.mean(values * values, axis=-1, keepdims=True) + 1e-06)
        normed = (values * scale * gain_ref[...]).astype(BF).reshape(groups // 2, rows // groups, width)
        for m in range(members):
            out_ref[c * groups // 2:(c + 1) * groups // 2, m] = normed


def selection(groups, members, slots, route_ref, gw_ref):
    rows = route_ref.shape[1]
    e0, e1 = route_ref[0:1, :], route_ref[1:2, :]
    rank = rank_in_group(e0 // members, groups)
    row = lax.broadcasted_iota(jnp.int32, (groups * members * slots, rows), 0)
    expert = row // slots
    weight = jnp.where(expert == e0, gw_ref[0:1, :], 0.0) + jnp.where(expert == e1, gw_ref[1:2, :], 0.0)
    weight = jnp.where(row % slots == rank, weight, 0.0).T
    high = weight.astype(BF)
    return jnp.concatenate([high, (weight - high.astype(F32)).astype(BF)], axis=0)


def expert_kernel(groups, members, x_ref, wg_ref, wu_ref, wd_ref, route_ref, gw_ref, out_ref, pick_ref):
    pick_ref[...] = selection(groups, members, x_ref.shape[1], route_ref, gw_ref)
    blocks, slots, width = x_ref.shape
    step = blocks // 2
    half = wg_ref.shape[1] // 2
    for c in range(2):
        x = x_ref[c * step:(c + 1) * step].reshape(step * slots, width)
        parts = []
        for n in range(2):
            gate = jnp.dot(x, wg_ref[:, n * half:(n + 1) * half], preferred_element_type=F32)
            up = jnp.dot(x, wu_ref[:, n * half:(n + 1) * half], preferred_element_type=F32)
            parts.append((gate / (1.0 + jnp.exp(-gate)) * up).astype(BF))
        hidden = jnp.concatenate(parts, axis=1)
        out = jnp.dot(hidden, wd_ref[...], preferred_element_type=F32).astype(BF)
        out_ref[c * step:(c + 1) * step] = out.reshape(step, slots, width)


def combine_kernel(r_ref, pick_ref, out_hbm, out_ref, sems):
    blocks, slots, width = r_ref.shape
    rows = out_ref.shape[0]
    parts = sems.shape[0]
    step = width // parts
    pick = pick_ref[...]
    copies = []
    for p in range(parts):
        span = pl.ds(p * step, step)
        r = r_ref[:, :, p * step:(p + 1) * step].reshape(blocks * slots, step)
        out = jnp.dot(pick, r, preferred_element_type=F32)
        out_ref[:, p * step:(p + 1) * step] = (out[:rows] + out[rows:]).astype(BF)
        copies.append(pltpu.make_async_copy(out_ref.at[:, span], out_hbm.at[:, span], sems.at[p]))
        copies[-1].start()
    for copy in copies:
        copy.wait()


def local(tokens, norm_gain, w_gate, w_up, w_down, routing, gate_weight):
    rows, width = tokens.shape
    groups = lax.axis_size("ep")
    members = lax.axis_size("tp")
    experts = groups * members
    slots = rows // groups
    route = routing.T
    weights = gate_weight.T
    params = pltpu.CompilerParams(vmem_limit_bytes=20 * 1024 * 1024)
    busy = pl.CostEstimate(flops=2_000_000_000, bytes_accessed=0, transcendentals=0)
    zero = pl.pallas_call(
        lead_kernel,
        out_shape=jax.ShapeDtypeStruct((8, rows), jnp.int32),
        compiler_params=params,
        cost_estimate=busy,
        name="lead",
    )()
    pick = pl.pallas_call(
        lambda *refs: slots_kernel(groups, members, *refs),
        out_shape=jax.ShapeDtypeStruct((rows, rows), BF),
        compiler_params=params,
        name="slots",
    )(zero, route)
    outgoing = pl.pallas_call(
        lambda *refs: dispatch_kernel(groups, members, *refs),
        out_shape=jax.ShapeDtypeStruct((groups, members, slots, width), BF),
        compiler_params=params,
        name="dispatch",
    )(pick, tokens, norm_gain.reshape(1, width))
    arrived = lax.all_to_all(outgoing.reshape(experts, slots, width), AXES, split_axis=0, concat_axis=0, tiled=True)
    in_vmem = pl.BlockSpec(memory_space=pltpu.VMEM)
    answered, weighted = pl.pallas_call(
        lambda *refs: expert_kernel(groups, members, *refs),
        in_specs=[in_vmem] * 6,
        out_specs=[in_vmem] * 2,
        out_shape=[
            jax.ShapeDtypeStruct((experts, slots, width), BF),
            jax.ShapeDtypeStruct((2 * rows, experts * slots), BF),
        ],
        compiler_params=params,
        name="expert",
    )(arrived, w_gate[0], w_up[0], w_down[0], route, weights)
    returned = lax.all_to_all(answered, AXES, split_axis=0, concat_axis=0, tiled=True)
    return pl.pallas_call(
        combine_kernel,
        in_specs=[in_vmem] * 2,
        out_specs=pl.BlockSpec(memory_space=pltpu.HBM),
        out_shape=jax.ShapeDtypeStruct((rows, width), BF),
        scratch_shapes=[pltpu.VMEM((rows, width), BF), pltpu.SemaphoreType.DMA((4,))],
        compiler_params=params,
        name="combine",
    )(returned, weighted)


def solution(mesh):
    placed = (
        P(AXES, None),
        P(),
        P(AXES, None, None),
        P(AXES, None, None),
        P(AXES, None, None),
        P(AXES, None),
        P(AXES, None),
    )
    return jax.shard_map(local, mesh=mesh, in_specs=placed, out_specs=P(AXES, None), check_vma=False)
```

```python
import jax
import jax.numpy as jnp
from jax import lax
from jax.experimental import pallas as pl
from jax.experimental.pallas import tpu as pltpu
from jax.sharding import Mesh, PartitionSpec as P

AXES = ("chip", "core", "tp")
ORDER = ("core", "chip", "tp")
CORES = 2
BF = jnp.bfloat16
F32 = jnp.float32


def rank_in_group(group, groups):
    n = group.shape[1]
    member = lax.broadcasted_iota(jnp.int32, (groups, n), 0) == group
    earlier = lax.broadcasted_iota(jnp.int32, (n, n), 0) < lax.broadcasted_iota(jnp.int32, (n, n), 1)
    counts = jnp.dot(member.astype(BF), earlier.astype(BF), preferred_element_type=F32)
    return jnp.sum(jnp.where(member, counts, 0.0), axis=0, keepdims=True).astype(jnp.int32)


def lead_kernel(out_ref):
    out_ref[...] = jnp.zeros(out_ref.shape, jnp.int32)


def slots_kernel(groups, members, cores, zero_ref, route_ref, pick_ref):
    rows = pick_ref.shape[0]
    group = (route_ref[0:1, :] + zero_ref[0:1, :]) // members
    block = group % cores * (groups // cores) + group // cores
    place = block * (rows // groups) + rank_in_group(group, groups)
    pick_ref[...] = (lax.broadcasted_iota(jnp.int32, (rows, rows), 0) == place).astype(BF)


def dispatch_kernel(groups, members, pick_ref, tok_ref, gain_ref, out_ref):
    rows, width = tok_ref.shape
    half = rows // 2
    for c in range(2):
        values = jnp.dot(pick_ref[c * half:(c + 1) * half], tok_ref[...], preferred_element_type=F32)
        scale = lax.rsqrt(jnp.mean(values * values, axis=-1, keepdims=True) + 1e-06)
        normed = (values * scale * gain_ref[...]).astype(BF).reshape(groups // 2, rows // groups, width)
        for m in range(members):
            out_ref[c * groups // 2:(c + 1) * groups // 2, m] = normed


def selection(groups, members, cores, slots, route_ref, gw_ref):
    rows = route_ref.shape[1]
    e0, e1 = route_ref[0:1, :], route_ref[1:2, :]
    rank = rank_in_group(e0 // members, groups)
    row = lax.broadcasted_iota(jnp.int32, (groups * members * slots, rows), 0)
    block = row // (slots * members)
    group = block % (groups // cores) * cores + block // (groups // cores)
    expert = group * members + row // slots % members
    weight = jnp.where(expert == e0, gw_ref[0:1, :], 0.0) + jnp.where(expert == e1, gw_ref[1:2, :], 0.0)
    weight = jnp.where(row % slots == rank, weight, 0.0).T
    high = weight.astype(BF)
    return jnp.concatenate([high, (weight - high.astype(F32)).astype(BF)], axis=0)


def expert_kernel(groups, members, cores, x_ref, wg_ref, wu_ref, wd_ref, route_ref, gw_ref, out_ref, pick_ref):
    pick_ref[...] = selection(groups, members, cores, x_ref.shape[1], route_ref, gw_ref)
    blocks, slots, width = x_ref.shape
    step = blocks // 2
    half = wg_ref.shape[1] // 2
    for c in range(2):
        x = x_ref[c * step:(c + 1) * step].reshape(step * slots, width)
        parts = []
        for n in range(2):
            gate = jnp.dot(x, wg_ref[:, n * half:(n + 1) * half], preferred_element_type=F32)
            up = jnp.dot(x, wu_ref[:, n * half:(n + 1) * half], preferred_element_type=F32)
            parts.append((gate / (1.0 + jnp.exp(-gate)) * up).astype(BF))
        hidden = jnp.concatenate(parts, axis=1)
        out = jnp.dot(hidden, wd_ref[...], preferred_element_type=F32).astype(BF)
        out_ref[c * step:(c + 1) * step] = out.reshape(step, slots, width)


def combine_kernel(r_ref, pick_ref, out_hbm, out_ref, sems):
    blocks, slots, width = r_ref.shape
    rows = out_ref.shape[0]
    parts = sems.shape[0]
    step = width // parts
    pick = pick_ref[...]
    copies = []
    for p in range(parts):
        span = pl.ds(p * step, step)
        r = r_ref[:, :, p * step:(p + 1) * step].reshape(blocks * slots, step)
        out = jnp.dot(pick, r, preferred_element_type=F32)
        out_ref[:, p * step:(p + 1) * step] = (out[:rows] + out[rows:]).astype(BF)
        copies.append(pltpu.make_async_copy(out_ref.at[:, span], out_hbm.at[:, span], sems.at[p]))
        copies[-1].start()
    for copy in copies:
        copy.wait()


def local(tokens, norm_gain, w_gate, w_up, w_down, routing, gate_weight):
    rows, width = tokens.shape
    cores = lax.axis_size("core")
    groups = lax.axis_size("chip") * cores
    members = lax.axis_size("tp")
    experts = groups * members
    slots = rows // groups
    route = routing.T
    weights = gate_weight.T
    params = pltpu.CompilerParams(vmem_limit_bytes=20 * 1024 * 1024)
    busy = pl.CostEstimate(flops=2_000_000_000, bytes_accessed=0, transcendentals=0)
    zero = pl.pallas_call(
        lead_kernel,
        out_shape=jax.ShapeDtypeStruct((8, rows), jnp.int32),
        compiler_params=params,
        cost_estimate=busy,
        name="lead",
    )()
    pick = pl.pallas_call(
        lambda *refs: slots_kernel(groups, members, cores, *refs),
        out_shape=jax.ShapeDtypeStruct((rows, rows), BF),
        compiler_params=params,
        name="slots",
    )(zero, route)
    outgoing = pl.pallas_call(
        lambda *refs: dispatch_kernel(groups, members, *refs),
        out_shape=jax.ShapeDtypeStruct((groups, members, slots, width), BF),
        compiler_params=params,
        name="dispatch",
    )(pick, tokens, norm_gain.reshape(1, width))
    arrived = lax.all_to_all(outgoing.reshape(experts, slots, width), ORDER, split_axis=0, concat_axis=0, tiled=True)
    in_vmem = pl.BlockSpec(memory_space=pltpu.VMEM)
    answered, weighted = pl.pallas_call(
        lambda *refs: expert_kernel(groups, members, cores, *refs),
        in_specs=[in_vmem] * 6,
        out_specs=[in_vmem] * 2,
        out_shape=[
            jax.ShapeDtypeStruct((experts, slots, width), BF),
            jax.ShapeDtypeStruct((2 * rows, experts * slots), BF),
        ],
        compiler_params=params,
        name="expert",
    )(arrived, w_gate[0], w_up[0], w_down[0], route, weights)
    returned = lax.all_to_all(answered, ORDER, split_axis=0, concat_axis=0, tiled=True)
    return pl.pallas_call(
        combine_kernel,
        in_specs=[in_vmem] * 2,
        out_specs=pl.BlockSpec(memory_space=pltpu.HBM),
        out_shape=jax.ShapeDtypeStruct((rows, width), BF),
        scratch_shapes=[pltpu.VMEM((rows, width), BF), pltpu.SemaphoreType.DMA((4,))],
        compiler_params=params,
        name="combine",
    )(returned, weighted)


def solution(mesh):
    shape = (mesh.shape["ep"] // CORES, CORES, mesh.shape["tp"])
    mesh = Mesh(mesh.devices.reshape(shape), AXES)
    placed = (
        P(AXES, None),
        P(),
        P(AXES, None, None),
        P(AXES, None, None),
        P(AXES, None, None),
        P(AXES, None),
        P(AXES, None),
    )
    return jax.shard_map(local, mesh=mesh, in_specs=placed, out_specs=P(AXES, None), check_vma=False)
```

```python
import jax
import jax.numpy as jnp
from jax import lax
from jax.experimental import pallas as pl
from jax.experimental.pallas import tpu as pltpu
from jax.sharding import Mesh, PartitionSpec as P

AXES = ("chip", "core", "tp")
ORDER = ("core", "chip", "tp")
CORES = 2
BF = jnp.bfloat16
F32 = jnp.float32


def rank_in_group(group, groups):
    n = group.shape[1]
    member = lax.broadcasted_iota(jnp.int32, (groups, n), 0) == group
    earlier = lax.broadcasted_iota(jnp.int32, (n, n), 0) < lax.broadcasted_iota(jnp.int32, (n, n), 1)
    counts = jnp.dot(member.astype(BF), earlier.astype(BF), preferred_element_type=F32)
    return jnp.sum(jnp.where(member, counts, 0.0), axis=0, keepdims=True).astype(jnp.int32)


def lead_kernel(out_ref):
    out_ref[...] = jnp.zeros(out_ref.shape, jnp.int32)


def slots_kernel(groups, members, cores, zero_ref, route_ref, pick_ref):
    rows = pick_ref.shape[0]
    group = (route_ref[0:1, :] + zero_ref[0:1, :]) // members
    block = group % cores * (groups // cores) + group // cores
    place = block * (rows // groups) + rank_in_group(group, groups)
    pick_ref[...] = (lax.broadcasted_iota(jnp.int32, (rows, rows), 0) == place).astype(BF)


def dispatch_kernel(groups, members, pick_ref, tok_ref, gain_ref, out_ref):
    rows, width = tok_ref.shape
    half = rows // 2
    for c in range(2):
        values = jnp.dot(pick_ref[c * half:(c + 1) * half], tok_ref[...], preferred_element_type=F32)
        scale = lax.rsqrt(jnp.mean(values * values, axis=-1, keepdims=True) + 1e-06)
        normed = (values * scale * gain_ref[...]).astype(BF).reshape(groups // 2, rows // groups, width)
        for m in range(members):
            out_ref[c * groups // 2:(c + 1) * groups // 2, m] = normed


def selection(groups, members, cores, slots, route_ref, gw_ref):
    rows = route_ref.shape[1]
    e0, e1 = route_ref[0:1, :], route_ref[1:2, :]
    rank = rank_in_group(e0 // members, groups)
    row = lax.broadcasted_iota(jnp.int32, (groups * members * slots, rows), 0)
    block = row // (slots * members)
    group = block % (groups // cores) * cores + block // (groups // cores)
    expert = group * members + row // slots % members
    weight = jnp.where(expert == e0, gw_ref[0:1, :], 0.0) + jnp.where(expert == e1, gw_ref[1:2, :], 0.0)
    weight = jnp.where(row % slots == rank, weight, 0.0).T
    high = weight.astype(BF)
    return jnp.concatenate([high, (weight - high.astype(F32)).astype(BF)], axis=0)


def expert_kernel(groups, members, cores, x_ref, wg_ref, wu_ref, wd_ref, route_ref, gw_ref, out_ref, pick_ref):
    pick_ref[...] = selection(groups, members, cores, x_ref.shape[1], route_ref, gw_ref)
    blocks, slots, width = x_ref.shape
    step = blocks // 2
    half = wg_ref.shape[1] // 2
    for c in range(2):
        x = x_ref[c * step:(c + 1) * step].reshape(step * slots, width)
        parts = []
        for n in range(2):
            gate = jnp.dot(x, wg_ref[:, n * half:(n + 1) * half], preferred_element_type=F32)
            up = jnp.dot(x, wu_ref[:, n * half:(n + 1) * half], preferred_element_type=F32)
            parts.append((gate / (1.0 + jnp.exp(-gate)) * up).astype(BF))
        hidden = jnp.concatenate(parts, axis=1)
        out = jnp.dot(hidden, wd_ref[...], preferred_element_type=F32).astype(BF)
        out_ref[c * step:(c + 1) * step] = out.reshape(step, slots, width)


def combine_kernel(r_ref, pick_ref, out_hbm, out_ref, sems):
    blocks, slots, width = r_ref.shape
    rows = out_ref.shape[0]
    pick = pick_ref[...]
    copies = []
    cut = width * 3 // 4
    for p, (at, step) in enumerate(((0, cut), (cut, width - cut))):
        span = pl.ds(at, step)
        r = r_ref[:, :, at:at + step].reshape(blocks * slots, step)
        out = jnp.dot(pick, r, preferred_element_type=F32)
        out_ref[:, at:at + step] = (out[:rows] + out[rows:]).astype(BF)
        copies.append(pltpu.make_async_copy(out_ref.at[:, span], out_hbm.at[:, span], sems.at[p]))
        copies[-1].start()
    for copy in copies:
        copy.wait()


def local(tokens, norm_gain, w_gate, w_up, w_down, routing, gate_weight):
    rows, width = tokens.shape
    cores = lax.axis_size("core")
    groups = lax.axis_size("chip") * cores
    members = lax.axis_size("tp")
    experts = groups * members
    slots = rows // groups
    route = routing.T
    weights = gate_weight.T
    params = pltpu.CompilerParams(vmem_limit_bytes=20 * 1024 * 1024)
    busy = pl.CostEstimate(flops=2_000_000_000, bytes_accessed=0, transcendentals=0)
    zero = pl.pallas_call(
        lead_kernel,
        out_shape=jax.ShapeDtypeStruct((8, rows), jnp.int32),
        compiler_params=params,
        cost_estimate=busy,
        name="lead",
    )()
    pick = pl.pallas_call(
        lambda *refs: slots_kernel(groups, members, cores, *refs),
        out_shape=jax.ShapeDtypeStruct((rows, rows), BF),
        compiler_params=params,
        name="slots",
    )(zero, route)
    outgoing = pl.pallas_call(
        lambda *refs: dispatch_kernel(groups, members, *refs),
        out_shape=jax.ShapeDtypeStruct((groups, members, slots, width), BF),
        compiler_params=params,
        name="dispatch",
    )(pick, tokens, norm_gain.reshape(1, width))
    arrived = lax.all_to_all(outgoing.reshape(experts, slots, width), ORDER, split_axis=0, concat_axis=0, tiled=True)
    in_vmem = pl.BlockSpec(memory_space=pltpu.VMEM)
    answered, weighted = pl.pallas_call(
        lambda *refs: expert_kernel(groups, members, cores, *refs),
        in_specs=[in_vmem] * 6,
        out_specs=[in_vmem] * 2,
        out_shape=[
            jax.ShapeDtypeStruct((experts, slots, width), BF),
            jax.ShapeDtypeStruct((2 * rows, experts * slots), BF),
        ],
        compiler_params=params,
        name="expert",
    )(arrived, w_gate[0], w_up[0], w_down[0], route, weights)
    returned = lax.all_to_all(answered, ORDER, split_axis=0, concat_axis=0, tiled=True)
    return pl.pallas_call(
        combine_kernel,
        in_specs=[in_vmem] * 2,
        out_specs=pl.BlockSpec(memory_space=pltpu.HBM),
        out_shape=jax.ShapeDtypeStruct((rows, width), BF),
        scratch_shapes=[pltpu.VMEM((rows, width), BF), pltpu.SemaphoreType.DMA((2,))],
        compiler_params=params,
        name="combine",
    )(returned, weighted)


def solution(mesh):
    shape = (mesh.shape["ep"] // CORES, CORES, mesh.shape["tp"])
    mesh = Mesh(mesh.devices.reshape(shape), AXES)
    placed = (
        P(AXES, None),
        P(),
        P(AXES, None, None),
        P(AXES, None, None),
        P(AXES, None, None),
        P(AXES, None),
        P(AXES, None),
    )
    return jax.shard_map(local, mesh=mesh, in_specs=placed, out_specs=P(AXES, None), check_vma=False)
```
